32 devices in a mesh: sp: 8 (over z, core), tp: 4 (over y, x).
Axes of the slice: x: 2, y: 2, z: 4, core: 2. Of those that a mesh axis runs over, the one named last changes fastest.
Arguments:
- residual_input: bfloat16 [1024, 2048], P(('sp', 'tp')), may hold values from -6 to 6
- mixer_value_input: bfloat16 [1024, 2048], P('sp', 'tp'), may hold values from -6 to 6
- gate_preactivation: bfloat16 [1024, 2048], P('sp', 'tp'), may hold values from -6 to 6
- state_projection_input: bfloat16 [1024, 2, 4, 128], P('sp'), may hold values from -6 to 6
- step_preactivation: bfloat16 [1024, 2, 32], P('sp', None, 'tp'), may hold values from -6 to 6
- spike_log_decay: float32 [1024, 2, 32], P('sp', None, 'tp'), may hold values from -1 to 0
- value_filter_taps: float32 [5, 2048], P(None, 'tp'), may hold values from -2.5 to 2.5
- state_projection_taps: float32 [5, 2, 4, 128], replicated, may hold values from -2.5 to 2.5
- step_size_bias: float32 [2, 32], P(None, 'tp'), may hold values from -0.5 to 0.5
- head_log_decay: float32 [2, 32], P(None, 'tp'), may hold values from -12 to -3
- gated_norm_gain: float32 [2048], P('tp'), may hold values from 0.1 to 1.9
- mixer_output_weight: bfloat16 [2048, 2048], P('tp'), may hold values from -0.125 to 0.125
- feedforward_norm_gain: float32 [2048], replicated, may hold values from 0.1 to 1.9
- routed_expert_index: int32 [1024, 4], P('sp'), may hold values from 0 to 7, all different within a row; in each aligned block of 128 rows (0 to 127, 128 to 255, ...) at most 96 rows name the same one
- routed_expert_weight: float32 [1024, 4], P('sp'), may hold values from 0.2 to 1.2
- routed_gate_weight: bfloat16 [8, 2048, 2048], P('sp', None, 'tp'), may hold values from -0.125 to 0.125
- routed_up_weight: bfloat16 [8, 2048, 2048], P('sp', None, 'tp'), may hold values from -0.125 to 0.125
- routed_down_weight: bfloat16 [8, 2048, 2048], P('sp', 'tp'), may hold values from -0.1875 to 0.1875
- common_gate_weight: bfloat16 [2048, 2048], P(None, 'tp'), may hold values from -0.125 to 0.125
- common_up_weight: bfloat16 [2048, 2048], P(None, 'tp'), may hold values from -0.125 to 0.125
- common_down_weight: bfloat16 [2048, 2048], P('tp'), may hold values from -0.125 to 0.125
Outputs:
- layer_out: bfloat16 [1024, 2048], P(('sp', 'tp'))
The draws below stay inside these ranges and needn't reach their ends.
Inputs may be any that keep to these rules, and one draw needn't show every extreme that they name: `routed_expert_index`: each row names 4 different experts. In the aligned blocks of 128 rows no expert is named by more than 96 rows, and in some block one expert is named by exactly 96.
All inputs are finite; a program needn't handle non-finite values.
Results may differ from the reference program's by a relative error of at most 0.02.
Values may be sent and summed in bfloat16 or wider, within the bound.
A program may use at most 64 MiB of HBM per device.

```python
import math
import jax
import jax.numpy as jnp
import numpy as np
from jax import lax

D = 2048
HEADS = 32
HD = 64
GROUPS = 4
STATE = 128
CONV = 5
BLK = 128
TOK_DEV = 128
TOP_K = 4
FF_E = 2048
FF_S = 2048
HW = 2048
TOKENS = 1024
EXPERTS = 8
CAP = 96
N_SP = 8
N_TP = 4


def draw_step_preactivation(key, part):
    noise_key, offset_key = jax.random.split(jax.random.fold_in(key, 11))
    noise = jnp.clip(jax.random.normal(noise_key, (TOKENS, 2, HEADS), jnp.float32), -4.0, 4.0)
    offsets = jax.random.uniform(offset_key, (TOKENS // TOK_DEV, 1, 1), jnp.float32, -1.5, 1.5)
    return (noise + jnp.repeat(offsets, TOK_DEV, axis=0)).astype(jnp.bfloat16)


def draw_head_log_decay(key, part):
    pick_key, fast_key, slow_key = jax.random.split(jax.random.fold_in(key, 23), 3)
    fast_heads = jax.random.randint(pick_key, (2, HEADS), 0, 2) == 0
    fast_rate = jax.random.uniform(fast_key, (2, HEADS), jnp.float32, math.log(1.0 / 80.0), math.log(1.0 / 25.0))
    slow_rate = jnp.log(jax.random.uniform(slow_key, (2, HEADS), jnp.float32, 0.1, 0.6) / TOKENS)
    return jnp.where(fast_heads, fast_rate, slow_rate).astype(jnp.float32)


def draw_spike_log_decay(key, part):
    spot_key, value_key = jax.random.split(jax.random.fold_in(key, 37))
    spike_positions = jax.random.randint(spot_key, (2, 2, HEADS), 0, TOKENS)
    decay_levels = jnp.log(jax.random.uniform(value_key, (2, 2, HEADS), jnp.float32, 0.5, 0.8))
    sequence_line = lax.broadcasted_iota(jnp.int32, (TOKENS, 2, HEADS), 0)
    final_result = jnp.zeros((TOKENS, 2, HEADS), jnp.float32)
    for decay_spike in range(2):
        final_result = final_result + jnp.where(sequence_line == spike_positions[decay_spike][None], decay_levels[decay_spike][None], 0.0)
    return final_result


def strengthened(result, own_key, source, target, parts, factor):
    owner, partner = [(jnp.arange(result.shape[axis_at]) // (result.shape[axis_at] // parts)).reshape([-1 if axis == axis_at else 1 for axis in range(result.ndim)]) for axis_at in (source, target)]
    chosen = jax.random.permutation(own_key, parts)[partner]
    strong = (owner == chosen) | (owner == (partner + parts // 2) % parts)
    return jnp.where(strong, factor * result, result)


def steps_of(own_key, dims, pieces, least, high):
    def one(dim, parts):
        heights = jax.random.uniform(jax.random.fold_in(jax.random.fold_in(own_key, 6), dim), (parts,), jnp.float32, least / len(pieces), high / len(pieces))
        return jnp.repeat(jnp.exp(heights), dims[dim] // parts).reshape((-1,) + (1,) * (len(dims) - dim - 1))

    factor_of = one(*pieces[0])
    for cut in pieces[1:]:
        factor_of = factor_of * one(*cut)
    return factor_of


def assign_block(stream_key, own, number, rows, number_of, top, bound, lean):
    sequence = jax.random.permutation(stream_key, number_of)
    crowded, usual = load_shares(number_of, rows * top, bound, lean, True), load_shares(number_of, rows * top, bound, lean, False)
    places = jnp.arange(number_of)

    def named(sizes, rotation):
        used = int((sizes > 0).sum())
        fixed = max(1, used // 4)
        passed = fixed + (places - fixed + rotation * (used - fixed)) % max(1, number_of - fixed)
        return jnp.zeros((number_of,), jnp.int32).at[sequence[jnp.where(places < fixed, places, passed)]].set(jnp.asarray(sizes, jnp.int32))

    sizes = jnp.where(number % 4 == 0, named(crowded, number // 4), named(usual, number - number // 4 - 1))
    mixed = jax.random.permutation(jax.random.fold_in(own, 3), number_of)
    donor, sink = mixed[0:number_of // 2 * 2:2], mixed[1:number_of // 2 * 2:2]
    slack = jnp.minimum(sizes[donor] - 1, bound - sizes[sink]) // 2
    slack = jnp.where((donor == sequence[0]) | (sink == sequence[0]) | (sizes[sink] == 0), 0, jnp.maximum(slack, 0))
    passed = jax.random.randint(jax.random.fold_in(own, 4), (number_of // 2,), 0, 1 << 20) % (slack + 1)
    sizes = sizes.at[donor].add(-passed).at[sink].add(passed)
    members = jnp.searchsorted(jnp.cumsum(sizes), jnp.arange(rows * top), side="right").astype(jnp.int32)
    listing = members.reshape(top, rows).T
    listing = listing[jax.random.permutation(jax.random.fold_in(own, 1), rows)]
    rotation = jax.random.randint(jax.random.fold_in(own, 2), (rows, 1), 0, top)
    return jnp.take_along_axis(listing, (jnp.arange(top)[None, :] + rotation) % top, axis=1)


def load_shares(number_of, total, most, slope, full):
    weights = [(1 << 20) // math.isqrt(standing ** slope) + 1 for standing in range(1, number_of + 1)]
    largest = most if full else min(most, max(-(-total // number_of), total * weights[0] // sum(weights)))
    least = 1 if total - largest >= number_of - 1 else 0
    holding, surplus = [largest] + [least] * (number_of - 1), total - largest - least * (number_of - 1)
    while surplus > 0:
        free = [i for i in range(1, number_of) if holding[i] < largest] or [i for i in range(1, number_of) if holding[i] < most]
        mass, left = sum([weights[i] for i in free]), surplus
        for i in free:
            addition = min(most - holding[i], max(1, left * weights[i] // mass), surplus)
            holding[i] = holding[i] + addition
            surplus = surplus - addition
    return np.array(holding)


def normal_values(key, extent, width, most, cuts=(), kind=jnp.bfloat16):
    values = width * jax.random.normal(key, extent, jnp.float32)
    if cuts:
        values = values * steps_of(key, extent, cuts, -0.22, 0.18)
    return jnp.clip(values, -most, most).astype(kind)


def heavy_noise(rng, extent, scale, bound, cuts, heavy, kind=jnp.bfloat16):
    result = scale * jax.random.normal(rng, extent, jnp.float32)
    if cuts:
        result = result * steps_of(rng, extent, cuts, -0.22, 0.18)
    return jnp.clip(strengthened(result, jax.random.fold_in(rng, 3), *heavy), -bound, bound).astype(kind)


def setup_inputs(seed: int = 0) -> dict:
    splits = jax.random.split(jax.random.key(seed), 22)
    residual_input = normal_values(splits[0], (TOKENS, D), 1.0, 6.0, ((0, 32),))
    mixer_value_input = normal_values(splits[1], (TOKENS, HW), 1.0, 6.0, ((0, 8), (1, 4)))
    gate_preactivation = normal_values(splits[2], (TOKENS, HW), 1.0, 6.0, ((0, 8), (1, 4)))
    state_projection_input = normal_values(splits[3], (TOKENS, 2, GROUPS, STATE), 1.0, 6.0, ((0, 8),))
    step_preactivation = draw_step_preactivation(jax.random.fold_in(splits[21], 71), 0)
    spike_log_decay = draw_spike_log_decay(jax.random.fold_in(splits[21], 71), 0)
    value_filter_taps = normal_values(splits[6], (CONV, HW), CONV ** -0.5, 2.5, ((1, 4),), jnp.float32)
    state_projection_taps = normal_values(splits[7], (CONV, 2, GROUPS, STATE), CONV ** -0.5, 2.5, (), jnp.float32)
    step_size_bias = jnp.clip(jax.random.uniform(splits[8], (2, HEADS), jnp.float32, -0.5, 0.5) * steps_of(splits[8], (2, HEADS), ((1, 4),), -0.4, 0.0), -0.5, 0.5)
    head_log_decay = draw_head_log_decay(jax.random.fold_in(splits[21], 71), 0)
    gated_norm_gain = jnp.clip(1.0 + 0.18 * jax.random.normal(splits[10], (HW,), jnp.float32), 0.1, 1.9)
    mixer_output_weight = normal_values(splits[11], (HW, D), HW ** -0.5, 0.125, ((0, 4),))
    feedforward_norm_gain = jnp.clip(1.0 + 0.18 * jax.random.normal(splits[12], (D,), jnp.float32), 0.1, 1.9)
    routed_expert_index_keys = jax.random.split(jax.random.fold_in(splits[13], 1), TOKENS // TOK_DEV)
    routed_expert_index_turns = jax.random.permutation(jax.random.fold_in(splits[13], 3), TOKENS // TOK_DEV)
    routed_expert_index = jax.vmap(lambda own, number: assign_block(jax.random.fold_in(splits[13], 2), own, number, TOK_DEV, EXPERTS, TOP_K, CAP, 1))(routed_expert_index_keys, routed_expert_index_turns).reshape((TOKENS, TOP_K))
    routed_expert_weight = jnp.clip(0.2 + 1 * jax.random.uniform(splits[14], (TOKENS, TOP_K), jnp.float32) ** steps_of(splits[14], (TOKENS, TOP_K), ((0, 8),), -0.2, 0.2), 0.2, 1.2)
    routed_gate_weight = normal_values(splits[15], (EXPERTS, D, FF_E), D ** -0.5, 0.125, ((0, 8), (2, 4)))
    routed_up_weight = normal_values(splits[16], (EXPERTS, D, FF_E), D ** -0.5, 0.125, ((0, 8), (2, 4)))
    routed_down_weight = heavy_noise(splits[17], (EXPERTS, FF_E, D), FF_E ** -0.5, 0.1875, ((0, 8), (1, 4)), (1, 2, 4, 2.0))
    common_gate_weight = normal_values(splits[18], (D, FF_S), D ** -0.5, 0.125, ((1, 4),))
    common_up_weight = normal_values(splits[19], (D, FF_S), D ** -0.5, 0.125, ((1, 4),))
    common_down_weight = normal_values(splits[20], (FF_S, D), FF_S ** -0.5, 0.125, ((0, 4),))
    return {"residual_input": residual_input, "mixer_value_input": mixer_value_input, "gate_preactivation": gate_preactivation, "state_projection_input": state_projection_input, "step_preactivation": step_preactivation, "spike_log_decay": spike_log_decay, "value_filter_taps": value_filter_taps, "state_projection_taps": state_projection_taps, "step_size_bias": step_size_bias, "head_log_decay": head_log_decay, "gated_norm_gain": gated_norm_gain, "mixer_output_weight": mixer_output_weight, "feedforward_norm_gain": feedforward_norm_gain, "routed_expert_index": routed_expert_index, "routed_expert_weight": routed_expert_weight, "routed_gate_weight": routed_gate_weight, "routed_up_weight": routed_up_weight, "routed_down_weight": routed_down_weight, "common_gate_weight": common_gate_weight, "common_up_weight": common_up_weight, "common_down_weight": common_down_weight}


EPSILON = 1e-06
HIGHEST = lax.Precision.HIGHEST

def rounded(values):
    return lax.optimization_barrier(values.astype(jnp.bfloat16)).astype(jnp.float32)

def block_pass(inputs, decay_logarithm, b_state, c_state, block_len):
    length, groups, per_group, head_dim = inputs.shape
    states = b_state.shape[-1]
    blocks = length // block_len
    inputs = inputs.reshape(blocks, block_len, groups, per_group, head_dim)
    decay_logarithm = decay_logarithm.reshape(blocks, block_len, groups, per_group)
    b_blocks = b_state.reshape(blocks, block_len, groups, states)
    c_blocks = c_state.reshape(blocks, block_len, groups, states)
    within = jnp.cumsum(decay_logarithm, axis=1)
    row_index = lax.broadcasted_iota(jnp.int32, (block_len, block_len), 0)
    col_index = lax.broadcasted_iota(jnp.int32, (block_len, block_len), 1)
    below_mask = (row_index >= col_index)[None, :, :, None, None]
    spread = within[:, :, None] - within[:, None, :]
    weights = jnp.where(below_mask, jnp.exp(jnp.where(below_mask, spread, 0.0)), 0.0)
    scores = jnp.einsum('cign,cjgn->cijg', c_blocks, b_blocks, precision=HIGHEST)
    output = jnp.einsum('cijgr,cjgrp->cigrp', scores[..., None] * weights, inputs, precision=HIGHEST)
    tail_decay = jnp.exp(within[:, -1:] - within)
    block_ends = jnp.einsum('cjgn,cjgrp->cgrpn', b_blocks, inputs * tail_decay[..., None], precision=HIGHEST)
    totals = within[:, -1]

    def carry_step(carried, pair_item):
        block_total, block_end = pair_item
        return (jnp.exp(block_total)[..., None, None] * carried + block_end, carried)
    zero_state = jnp.zeros((groups, per_group, head_dim, states), jnp.float32)
    last_state, starts = lax.scan(carry_step, zero_state, (totals, block_ends))
    output = output + jnp.einsum('cign,cgrpn->cigrp', c_blocks, starts, precision=HIGHEST) * jnp.exp(within)[..., None]
    offsets = jnp.cumsum(totals, axis=0) - totals
    through = (within + offsets[:, None]).reshape(length, groups, per_group)
    return (output.reshape(length, groups, per_group, head_dim), lax.optimization_barrier(jnp.sum(totals, axis=0)), last_state, through)

def slot_table(expert_ids, experts, capacity):
    row_count, top_count = expert_ids.shape
    flat_ids = expert_ids.reshape(-1)
    one_hot = (flat_ids[:, None] == jnp.arange(experts, dtype=jnp.int32)[None, :]).astype(jnp.int32)
    earlier = jnp.cumsum(one_hot, axis=0) - one_hot
    position = lax.optimization_barrier(jnp.sum(earlier * one_hot, axis=1)).astype(jnp.int32)
    owners = (jnp.arange(row_count * top_count, dtype=jnp.int32) // top_count).astype(jnp.int32)
    table = jnp.full((experts * capacity,), row_count, jnp.int32).at[flat_ids * capacity + position].set(owners)
    return (position.reshape(row_count, top_count), table)

def blocked_sum(hidden, down):
    width_slice = down.shape[0] // N_TP

    def add_block(index, total):
        start = (index * width_slice).astype(jnp.int32)
        left = lax.dynamic_slice_in_dim(hidden, start, width_slice, 1)
        right = lax.dynamic_slice_in_dim(down, start, width_slice, 0)
        return total + rounded(jnp.dot(left, right, preferred_element_type=jnp.float32))
    return lax.fori_loop(0, N_TP, add_block, jnp.zeros((hidden.shape[0], down.shape[1]), jnp.float32))

def reference(residual_input, mixer_value_input, gate_preactivation, state_projection_input, step_preactivation, spike_log_decay, value_filter_taps, state_projection_taps, step_size_bias, head_log_decay, gated_norm_gain, mixer_output_weight, feedforward_norm_gain, routed_expert_index, routed_expert_weight, routed_gate_weight, routed_up_weight, routed_down_weight, common_gate_weight, common_up_weight, common_down_weight):
    seq_rows, mixer_cols = mixer_value_input.shape
    head_count = mixer_cols // HD
    groups, states = (state_projection_input.shape[2], state_projection_input.shape[3])
    per_group = head_count // groups
    taps = value_filter_taps.shape[0]
    margin = taps // 2
    joined = jnp.concatenate([mixer_value_input.astype(jnp.float32), state_projection_input.astype(jnp.float32).reshape(seq_rows, 2 * groups * states)], axis=1)
    kernel = jnp.concatenate([value_filter_taps, state_projection_taps.reshape(taps, 2 * groups * states)], axis=1)
    padded = jnp.pad(joined, ((margin, margin), (0, 0)))
    conv_out = jnp.zeros(joined.shape, jnp.float32)
    for offset in range(taps):
        conv_out = conv_out + kernel[offset] * padded[offset:offset + seq_rows]
    active = jax.nn.silu(conv_out)
    mixer_values = active[:, :mixer_cols].reshape(seq_rows, groups, per_group, HD)
    state_parts = active[:, mixer_cols:].reshape(seq_rows, 2, groups, states)
    b_state, c_state = (state_parts[:, 0], state_parts[:, 1])
    discrete_step_size = jax.nn.softplus(step_preactivation.astype(jnp.float32) + step_size_bias)
    decay_logarithm = spike_log_decay - discrete_step_size * jnp.exp(head_log_decay)
    forward_in = mixer_values * discrete_step_size[:, 0].reshape(seq_rows, groups, per_group)[..., None]
    backward_in = mixer_values * discrete_step_size[:, 1].reshape(seq_rows, groups, per_group)[..., None]
    forward_out = block_pass(forward_in, decay_logarithm[:, 0].reshape(seq_rows, groups, per_group), b_state, c_state, BLK)[0]
    backward_out = block_pass(jnp.flip(backward_in, 0), jnp.flip(decay_logarithm[:, 1].reshape(seq_rows, groups, per_group), 0), jnp.flip(b_state, 0), jnp.flip(c_state, 0), BLK)[0]
    scanned = (forward_out + jnp.flip(backward_out, 0)).reshape(seq_rows, mixer_cols)
    gated = (scanned * jax.nn.silu(gate_preactivation.astype(jnp.float32))).reshape(seq_rows, head_count, HD)
    gated = gated * lax.rsqrt(lax.optimization_barrier(jnp.mean(gated * gated, axis=-1, keepdims=True)) + EPSILON)
    mixed = (gated.reshape(seq_rows, mixer_cols) * gated_norm_gain).astype(jnp.bfloat16)
    projected = blocked_sum(mixed, mixer_output_weight)
    residual = (residual_input.astype(jnp.float32) + projected).astype(jnp.bfloat16)
    widened = residual.astype(jnp.float32)
    normed = (widened * lax.rsqrt(lax.optimization_barrier(jnp.mean(widened * widened, axis=-1, keepdims=True)) + EPSILON) * feedforward_norm_gain).astype(jnp.bfloat16)
    model_width = normed.shape[1]
    shared_hidden = (jax.nn.silu(jnp.dot(normed, common_gate_weight, preferred_element_type=jnp.float32)) * jnp.dot(normed, common_up_weight, preferred_element_type=jnp.float32)).astype(jnp.bfloat16)
    shared_out = blocked_sum(shared_hidden, common_down_weight)
    block_rows = seq_rows // N_SP
    experts = routed_gate_weight.shape[0]
    top_count = routed_expert_index.shape[1]
    capacity = 3 * block_rows * top_count // (2 * experts)
    id_blocks = routed_expert_index.reshape(N_SP, block_rows, top_count)
    weight_blocks = routed_expert_weight.reshape(N_SP, block_rows, top_count)

    def block_tables(block_ids, block_weights):
        position, table = slot_table(block_ids, experts, capacity)
        slot_index = block_ids.reshape(-1) * capacity + position.reshape(-1)
        slot_weight = jnp.zeros((experts * capacity,), jnp.float32).at[slot_index].set(block_weights.reshape(-1))
        return (table, slot_weight)
    tables, slot_weights = jax.vmap(block_tables)(id_blocks, weight_blocks)
    offsets = (jnp.arange(N_SP, dtype=jnp.int32) * block_rows)[:, None]
    global_rows = jnp.where(tables < block_rows, tables + offsets, seq_rows).astype(jnp.int32)
    expert_rows = global_rows.reshape(N_SP, experts, capacity).transpose(1, 0, 2).reshape(experts, N_SP * capacity)
    expert_weights = slot_weights.reshape(N_SP, experts, capacity).transpose(1, 0, 2).reshape(experts, N_SP * capacity)
    padded_norm = jnp.concatenate([normed, jnp.zeros((1, model_width), jnp.bfloat16)], axis=0)

    def expert_step(total, pair_item):
        gate_mat, up_mat, down_mat, rows_index, slot_weight = pair_item
        arrived = padded_norm[rows_index]
        hidden = (jax.nn.silu(jnp.dot(arrived, gate_mat, preferred_element_type=jnp.float32)) * jnp.dot(arrived, up_mat, preferred_element_type=jnp.float32)).astype(jnp.bfloat16)
        out_rows = blocked_sum(hidden, down_mat)
        return (total.at[rows_index].add(slot_weight[:, None] * out_rows), None)
    routed, _ = lax.scan(expert_step, jnp.zeros((seq_rows + 1, model_width), jnp.float32), (routed_gate_weight, routed_up_weight, routed_down_weight, expert_rows, expert_weights))
    feed = shared_out + routed[:seq_rows]
    return (widened + feed).astype(jnp.bfloat16)
```

```python
import functools

import jax
import jax.numpy as jnp
from jax import lax
from jax.experimental import pallas as pl
from jax.experimental.pallas import tpu as pltpu
from jax.sharding import PartitionSpec as P

HD = 64
EPSILON = 1e-06
HIGHEST = lax.Precision.HIGHEST
MESH = pl.DeviceIdType.MESH
F32 = jnp.float32
BF16 = jnp.bfloat16
EDGE = 16


def exact_dot(a, b, contract):
    return lax.dot_general(
        a, b, (contract, ((), ())), precision=HIGHEST, preferred_element_type=F32
    )


def narrow_dot(a, b, contract=((1,), (0,))):
    return lax.dot_general(
        a.astype(BF16), b.astype(BF16), (contract, ((), ())), preferred_element_type=F32
    )


def mixer_kernel(
    n,
    parts,
    groups,
    joined_ref,
    taps_ref,
    pre_ref,
    spike_ref,
    bias_ref,
    rate_ref,
    gate_ref,
    gain_ref,
    wout_ref,
    resid_ref,
    fgain_ref,
    route_ref,
    resid_out,
    normed_out,
    route_out,
    halo,
    ends,
    got,
    part,
    part_got,
    halo_send,
    halo_recv,
    state_send,
    state_recv,
    part_send,
    part_recv,
    route_send,
    route_recv,
    local_sem,
):
    d = lax.axis_index("sp")
    me = lax.axis_index("tp")
    length, width = gate_ref.shape
    heads = width // HD
    total_cols = joined_ref.shape[1]
    states = (total_cols - width) // (2 * groups)
    taps = taps_ref.shape[0]
    margin = taps // 2
    rows = length // parts
    barrier = pltpu.get_barrier_semaphore()
    for k in range(1, n):
        pl.semaphore_signal(
            barrier, inc=1, device_id={"sp": lax.rem(d + k, n)}, device_id_type=MESH
        )
    for k in range(1, parts):
        pl.semaphore_signal(
            barrier, inc=1, device_id={"tp": lax.rem(me + k, parts)}, device_id_type=MESH
        )
    pl.semaphore_wait(barrier, n + parts - 2)

    down = pltpu.make_async_remote_copy(
        src_ref=joined_ref.at[pl.ds(length - EDGE, EDGE)],
        dst_ref=halo.at[0],
        send_sem=halo_send.at[0],
        recv_sem=halo_recv.at[0],
        device_id={"sp": lax.rem(d + 1, n)},
        device_id_type=MESH,
    )
    up = pltpu.make_async_remote_copy(
        src_ref=joined_ref.at[pl.ds(0, EDGE)],
        dst_ref=halo.at[1],
        send_sem=halo_send.at[1],
        recv_sem=halo_recv.at[1],
        device_id={"sp": lax.rem(d + n - 1, n)},
        device_id_type=MESH,
    )
    down.start()
    up.start()
    route_copies = []
    for k in range(1, n):
        copy = pltpu.make_async_remote_copy(
            src_ref=route_ref,
            dst_ref=route_out.at[d],
            send_sem=route_send.at[k - 1],
            recv_sem=route_recv.at[k - 1],
            device_id={"sp": lax.rem(d + k, n)},
            device_id_type=MESH,
        )
        copy.start()
        route_copies.append(copy)
    own_route = pltpu.make_async_copy(route_ref, route_out.at[d], local_sem)
    own_route.start()

    pre = pre_ref[...] + bias_ref[...]
    step = jnp.maximum(pre, 0.0) + jnp.log1p(jnp.exp(-jnp.abs(pre)))
    decay = spike_ref[...] - step * jnp.exp(rate_ref[...])
    row_i = lax.broadcasted_iota(jnp.int32, (length, length), 0)
    col_i = lax.broadcasted_iota(jnp.int32, (length, length), 1)
    upto = jnp.where(row_i >= col_i, 1.0, 0.0).astype(F32)
    ones = jnp.ones((8, length), F32)
    eye = jnp.where(row_i == col_i, 1.0, 0.0).astype(F32)
    within = exact_dot(upto, decay, ((1,), (0,)))
    before = within - decay
    total = exact_dot(ones, decay, ((1,), (0,)))[0:1]
    within_t = exact_dot(within, eye, ((0,), (0,)))
    before_t = exact_dot(before, eye, ((0,), (0,)))
    step_t = exact_dot(step, eye, ((0,), (0,)))
    spread_head = lax.broadcasted_iota(jnp.int32, (heads, width), 0)
    spread_col = lax.broadcasted_iota(jnp.int32, (heads, width), 1)
    spread = jnp.where(spread_col // HD == spread_head, 1.0, 0.0).astype(F32)

    def widen(cells):
        return exact_dot(cells, spread, ((1,), (0,)))

    wf, ef = within[:, :heads], before[:, heads:]
    tf, tb = total[:, :heads], total[:, heads:]
    tail_f = widen(step[:, :heads] * jnp.exp(tf - wf))
    tail_b = widen(step[:, heads:] * jnp.exp(ef))
    head_f = widen(jnp.exp(wf))
    head_b = widen(jnp.exp(tb - ef))
    eight = jnp.zeros((8, heads), F32)
    total_f = widen(eight + tf)[0:1]
    total_b = widen(eight + tb)[0:1]

    down.wait()
    up.wait()
    previous = jnp.where(d > 0, halo[0].astype(F32), 0.0)
    following = jnp.where(d < n - 1, halo[1].astype(F32), 0.0)
    padded = jnp.concatenate([previous, joined_ref[...].astype(F32), following], axis=0)
    extent = length + 2 * EDGE
    conv = jnp.zeros((length, total_cols), F32)
    for k in range(taps):
        shift = (margin - k) % extent
        moved = pltpu.roll(padded, shift, 0) if shift else padded
        conv = conv + taps_ref[k : k + 1, :] * moved[EDGE : EDGE + length]
    act = conv * jax.nn.sigmoid(conv)
    values = act[:, :width]
    bs = [act[:, width + g * states : width + (g + 1) * states].astype(BF16) for g in range(groups)]
    cs = [
        act[:, width + (groups + g) * states : width + (groups + g + 1) * states].astype(BF16)
        for g in range(groups)
    ]
    share = width // groups
    end_row = lax.broadcasted_iota(jnp.int32, (EDGE, width), 0)
    for way, tail, tot in ((0, tail_f, total_f), (1, tail_b, total_b)):
        weighted = (values * tail).astype(BF16)
        for g in range(groups):
            cols = slice(g * share, (g + 1) * share)
            ends[way, 0:states, cols] = narrow_dot(bs[g], weighted[:, cols], ((0,), (0,))).astype(
                BF16
            )
        high = tot.astype(BF16).astype(F32)
        low = tot - high
        ends[way, states : states + EDGE, :] = jnp.where(
            end_row == 0, high, jnp.where(end_row == 1, low, 0.0)
        ).astype(BF16)
    state_copies = []
    for k in range(1, n):
        copy = pltpu.make_async_remote_copy(
            src_ref=ends.at[(d + k) // n],
            dst_ref=got.at[k - 1],
            send_sem=state_send.at[k - 1],
            recv_sem=state_recv.at[k - 1],
            device_id={"sp": lax.rem(d + k, n)},
            device_id_type=MESH,
        )
        copy.start()
        state_copies.append(copy)

    blocks = []
    heads_in = heads // groups
    for g in range(groups):
        scores = narrow_dot(cs[g], bs[g], ((1,), (1,)))
        for h in range(g * heads_in, (g + 1) * heads_in):
            b = heads + h
            spread_f = within[:, h : h + 1] - within_t[h : h + 1, :]
            spread_b = before_t[b : b + 1, :] - before[:, b : b + 1]
            factor = jnp.exp(jnp.where(row_i >= col_i, spread_f, spread_b))
            sf, sb = step_t[h : h + 1, :], step_t[b : b + 1, :]
            coeff = jnp.where(row_i >= col_i, sf, 0.0) + jnp.where(row_i <= col_i, sb, 0.0)
            mat = (scores * factor * coeff).astype(BF16)
            blocks.append(narrow_dot(mat, values[:, h * HD : (h + 1) * HD]))
    out = jnp.concatenate(blocks, axis=1)
    gate = gate_ref[...].astype(F32)
    gate = gate * jax.nn.sigmoid(gate)

    for copy in state_copies:
        copy.wait()
    weight = jnp.where(d >= 1, 1.0, 0.0) * jnp.ones((1, width), F32)
    start_f = jnp.zeros((states, width), F32)
    for k in range(1, n):
        weight = jnp.where(d >= k, weight, 0.0)
        start_f = start_f + weight * got[k - 1, 0:states, :].astype(F32)
        marks = got[k - 1, states : states + EDGE, :].astype(F32)
        weight = weight * jnp.exp(marks[0:1] + marks[1:2])
    weight = jnp.ones((1, width), F32)
    start_b = jnp.zeros((states, width), F32)
    for m in range(1, n):
        weight = jnp.where(d + m < n, weight, 0.0)
        slot = n - m - 1
        start_b = start_b + weight * got[slot, 0:states, :].astype(F32)
        marks = got[slot, states : states + EDGE, :].astype(F32)
        weight = weight * jnp.exp(jnp.minimum(marks[0:1] + marks[1:2], 0.0))
    carried = []
    for g in range(groups):
        cols = slice(g * share, (g + 1) * share)
        carried.append(
            head_f[:, cols] * narrow_dot(cs[g], start_f[:, cols])
            + head_b[:, cols] * narrow_dot(cs[g], start_b[:, cols])
        )
    out = out + (carried[0] if groups == 1 else jnp.concatenate(carried, axis=1))
    gated = out * gate
    square = exact_dot(gated * gated, spread, ((1,), (1,))) * (1.0 / HD)
    scale = widen(lax.rsqrt(square + EPSILON))
    mixed = (gated * scale * gain_ref[...]).astype(BF16)
    model = wout_ref.shape[1]
    tile = min(512, model)
    for c in range(0, model, tile):
        part[:, c : c + tile] = jnp.dot(
            mixed, wout_ref[:, c : c + tile], preferred_element_type=F32
        ).astype(BF16)
    part_copies = []
    for k in range(1, parts):
        target = lax.rem(me + k, parts)
        copy = pltpu.make_async_remote_copy(
            src_ref=part.at[pl.ds(pl.multiple_of(target * rows, rows), rows)],
            dst_ref=part_got.at[k - 1],
            send_sem=part_send.at[k - 1],
            recv_sem=part_recv.at[k - 1],
            device_id={"tp": target},
            device_id_type=MESH,
        )
        copy.start()
        part_copies.append(copy)
    residual = resid_ref[...].astype(F32) + part[
        pl.ds(pl.multiple_of(me * rows, rows), rows), :
    ].astype(F32)
    for k in range(1, parts):
        part_copies[k - 1].wait()
        residual = residual + part_got[k - 1].astype(F32)
    residual = residual.astype(BF16)
    resid_out[...] = residual
    wide = residual.astype(F32)
    mean = jnp.mean(wide * wide, axis=1, keepdims=True)
    normed_out[...] = (wide * lax.rsqrt(mean + EPSILON) * fgain_ref[...]).astype(BF16)
    own_route.wait()
    for copy in route_copies:
        copy.wait()


def on_device(
    residual_input,
    mixer_value_input,
    gate_preactivation,
    state_projection_input,
    step_preactivation,
    spike_log_decay,
    value_filter_taps,
    state_projection_taps,
    step_size_bias,
    head_log_decay,
    gated_norm_gain,
    mixer_output_weight,
    feedforward_norm_gain,
    routed_expert_index,
    routed_expert_weight,
    routed_gate_weight,
    routed_up_weight,
    routed_down_weight,
    common_gate_weight,
    common_up_weight,
    common_down_weight,
):
    n, parts = (lax.axis_size("sp"), lax.axis_size("tp"))
    seq_rows, width = mixer_value_input.shape
    heads = width // HD
    all_groups, states = state_projection_input.shape[2:]
    per_group = heads * parts // all_groups
    groups = max(1, heads // per_group)
    first_group = lax.axis_index("tp") * heads // per_group
    taps = value_filter_taps.shape[0]
    model = mixer_output_weight.shape[1]
    rows = residual_input.shape[0]
    local_experts = routed_gate_weight.shape[0]
    experts = local_experts * n
    bc = lax.dynamic_slice_in_dim(state_projection_input, first_group, groups, 2)
    bc_taps = lax.dynamic_slice_in_dim(state_projection_taps, first_group, groups, 2)
    joined = jnp.concatenate(
        [mixer_value_input, bc.reshape(seq_rows, 2 * groups * states)], axis=1
    )
    kernel = jnp.concatenate(
        [value_filter_taps, bc_taps.reshape(taps, 2 * groups * states)], axis=1
    )
    named = routed_expert_index[None] == jnp.arange(experts, dtype=jnp.int32)[:, None, None]
    route = jnp.sum(jnp.where(named, routed_expert_weight[None], 0.0), axis=2)
    cols = joined.shape[1]
    vmem = pl.BlockSpec(memory_space=pltpu.VMEM)
    dma = pltpu.SemaphoreType.DMA
    residual, normed, routes = pl.pallas_call(
        functools.partial(mixer_kernel, n, parts, groups),
        out_shape=(
            jax.ShapeDtypeStruct((rows, model), BF16),
            jax.ShapeDtypeStruct((rows, model), BF16),
            jax.ShapeDtypeStruct((n, experts, seq_rows), F32),
        ),
        in_specs=[vmem] * 12,
        out_specs=(vmem, vmem, vmem),
        scratch_shapes=[
            pltpu.VMEM((2, EDGE, cols), BF16),
            pltpu.VMEM((2, states + EDGE, width), BF16),
            pltpu.VMEM((n - 1, states + EDGE, width), BF16),
            pltpu.VMEM((seq_rows, model), BF16),
            pltpu.VMEM((parts - 1, rows, model), BF16),
            dma((2,)),
            dma((2,)),
            dma((n - 1,)),
            dma((n - 1,)),
            dma((parts - 1,)),
            dma((parts - 1,)),
            dma((n - 1,)),
            dma((n - 1,)),
            dma,
        ],
        compiler_params=pltpu.CompilerParams(collective_id=0, has_side_effects=True),
        name="mixer",
    )(
        joined,
        kernel,
        step_preactivation.astype(F32).reshape(seq_rows, 2 * heads),
        spike_log_decay.reshape(seq_rows, 2 * heads),
        step_size_bias.reshape(1, 2 * heads),
        head_log_decay.reshape(1, 2 * heads),
        gate_preactivation,
        gated_norm_gain.reshape(1, width),
        mixer_output_weight,
        residual_input,
        feedforward_norm_gain.reshape(1, model),
        route,
    )
    d = lax.axis_index("sp")
    every = lax.all_gather(normed, ("sp", "tp"), axis=0, tiled=True)
    mine = lax.dynamic_slice_in_dim(every, d * seq_rows, seq_rows, 0)

    def ffn(x, wg, wu, wd, scale):
        gate = jnp.dot(x, wg, preferred_element_type=F32)
        up = jnp.dot(x, wu, preferred_element_type=F32)
        hidden = jax.nn.silu(gate) * up
        if scale is not None:
            hidden = hidden * scale
        return jnp.dot(hidden.astype(BF16), wd, preferred_element_type=F32)

    shared = ffn(mine, common_gate_weight, common_up_weight, common_down_weight, None)
    here = (jnp.arange(n, dtype=jnp.int32) == d)[:, None, None]
    partial = jnp.where(here, shared[None], 0.0)
    for e in range(local_experts):
        scale = lax.dynamic_index_in_dim(routes, d * local_experts + e, 1, keepdims=False)
        partial = partial + ffn(
            every,
            routed_gate_weight[e],
            routed_up_weight[e],
            routed_down_weight[e],
            scale.reshape(n * seq_rows, 1),
        ).reshape(n, seq_rows, model)
    feed = lax.psum_scatter(
        partial.astype(BF16).reshape(n * seq_rows, model),
        ("sp", "tp"),
        scatter_dimension=0,
        tiled=True,
    )
    return (residual.astype(F32) + feed.astype(F32)).astype(BF16)


def solution(mesh):
    return jax.shard_map(
        on_device,
        mesh=mesh,
        in_specs=(
            P(("sp", "tp"), None),
            P("sp", "tp"),
            P("sp", "tp"),
            P("sp", None, None, None),
            P("sp", None, "tp"),
            P("sp", None, "tp"),
            P(None, "tp"),
            P(),
            P(None, "tp"),
            P(None, "tp"),
            P("tp"),
            P("tp", None),
            P(),
            P("sp", None),
            P("sp", None),
            P("sp", None, "tp"),
            P("sp", None, "tp"),
            P("sp", "tp", None),
            P(None, "tp"),
            P(None, "tp"),
            P("tp", None),
        ),
        out_specs=P(("sp", "tp"), None),
        check_vma=False,
    )
```

```python
import functools

import jax
import jax.numpy as jnp
from jax import lax
from jax.experimental import pallas as pl
from jax.experimental.pallas import tpu as pltpu
from jax.sharding import PartitionSpec as P

HD = 64
EPSILON = 1e-06
HIGHEST = lax.Precision.HIGHEST
MESH = pl.DeviceIdType.MESH
F32 = jnp.float32
BF16 = jnp.bfloat16
EDGE = 16


def exact_dot(a, b, contract):
    return lax.dot_general(
        a, b, (contract, ((), ())), precision=HIGHEST, preferred_element_type=F32
    )


def narrow_dot(a, b, contract=((1,), (0,))):
    return lax.dot_general(
        a.astype(BF16), b.astype(BF16), (contract, ((), ())), preferred_element_type=F32
    )


def mixer_kernel(
    n,
    parts,
    groups,
    joined_ref,
    value_taps_ref,
    state_taps_ref,
    pre_ref,
    spike_ref,
    bias_ref,
    rate_ref,
    gate_ref,
    gain_ref,
    wout_ref,
    resid_ref,
    fgain_ref,
    route_ref,
    resid_out,
    normed_out,
    route_out,
    halo,
    ends,
    got,
    part,
    part_got,
    halo_send,
    halo_recv,
    state_send,
    state_recv,
    part_send,
    part_recv,
    route_send,
    route_recv,
    local_sem,
):
    d = lax.axis_index("sp")
    me = lax.axis_index("tp")
    length, width = gate_ref.shape
    heads = width // HD
    total_cols = joined_ref.shape[1]
    states = (total_cols - width) // (2 * groups)
    taps = value_taps_ref.shape[0]
    margin = taps // 2
    rows = length // parts
    barrier = pltpu.get_barrier_semaphore()
    for k in range(1, n):
        pl.semaphore_signal(
            barrier, inc=1, device_id={"sp": lax.rem(d + k, n)}, device_id_type=MESH
        )
    for k in range(1, parts):
        pl.semaphore_signal(
            barrier, inc=1, device_id={"tp": lax.rem(me + k, parts)}, device_id_type=MESH
        )
    pl.semaphore_wait(barrier, n + parts - 2)

    down = pltpu.make_async_remote_copy(
        src_ref=joined_ref.at[pl.ds(length - EDGE, EDGE)],
        dst_ref=halo.at[0],
        send_sem=halo_send.at[0],
        recv_sem=halo_recv.at[0],
        device_id={"sp": lax.rem(d + 1, n)},
        device_id_type=MESH,
    )
    up = pltpu.make_async_remote_copy(
        src_ref=joined_ref.at[pl.ds(0, EDGE)],
        dst_ref=halo.at[1],
        send_sem=halo_send.at[1],
        recv_sem=halo_recv.at[1],
        device_id={"sp": lax.rem(d + n - 1, n)},
        device_id_type=MESH,
    )
    down.start()
    up.start()
    route_copies = []
    for k in range(1, n):
        copy = pltpu.make_async_remote_copy(
            src_ref=route_ref,
            dst_ref=route_out.at[d],
            send_sem=route_send.at[k - 1],
            recv_sem=route_recv.at[k - 1],
            device_id={"sp": lax.rem(d + k, n)},
            device_id_type=MESH,
        )
        copy.start()
        route_copies.append(copy)
    own_route = pltpu.make_async_copy(route_ref, route_out.at[d], local_sem)
    own_route.start()

    bias = jnp.concatenate([bias_ref[0:1, :], bias_ref[1:2, :]], axis=1)
    rate = jnp.concatenate([rate_ref[0:1, :], rate_ref[1:2, :]], axis=1)
    pre = pre_ref[...] + bias
    step = jnp.maximum(pre, 0.0) + jnp.log1p(jnp.exp(-jnp.abs(pre)))
    decay = spike_ref[...] - step * jnp.exp(rate)
    row_i = lax.broadcasted_iota(jnp.int32, (length, length), 0)
    col_i = lax.broadcasted_iota(jnp.int32, (length, length), 1)
    upto = jnp.where(row_i >= col_i, 1.0, 0.0).astype(F32)
    ones = jnp.ones((8, length), F32)
    eye = jnp.where(row_i == col_i, 1.0, 0.0).astype(F32)
    within = exact_dot(upto, decay, ((1,), (0,)))
    before = within - decay
    total = exact_dot(ones, decay, ((1,), (0,)))[0:1]
    within_t = exact_dot(within, eye, ((0,), (0,)))
    before_t = exact_dot(before, eye, ((0,), (0,)))
    step_t = exact_dot(step, eye, ((0,), (0,)))
    spread_head = lax.broadcasted_iota(jnp.int32, (heads, width), 0)
    spread_col = lax.broadcasted_iota(jnp.int32, (heads, width), 1)
    spread = jnp.where(spread_col // HD == spread_head, 1.0, 0.0).astype(F32)

    def widen(cells):
        return exact_dot(cells, spread, ((1,), (0,)))

    wf, ef = within[:, :heads], before[:, heads:]
    tf, tb = total[:, :heads], total[:, heads:]
    tail_f = widen(step[:, :heads] * jnp.exp(tf - wf))
    tail_b = widen(step[:, heads:] * jnp.exp(ef))
    head_f = widen(jnp.exp(wf))
    head_b = widen(jnp.exp(tb - ef))
    eight = jnp.zeros((8, heads), F32)
    total_f = widen(eight + tf)[0:1]
    total_b = widen(eight + tb)[0:1]

    down.wait()
    up.wait()
    previous = jnp.where(d > 0, halo[0].astype(F32), 0.0)
    following = jnp.where(d < n - 1, halo[1].astype(F32), 0.0)
    padded = jnp.concatenate([previous, joined_ref[...].astype(F32), following], axis=0)
    extent = length + 2 * EDGE
    filters = jnp.concatenate([value_taps_ref[...], state_taps_ref[...]], axis=1)
    conv = jnp.zeros((length, total_cols), F32)
    for k in range(taps):
        shift = (margin - k) % extent
        moved = pltpu.roll(padded, shift, 0) if shift else padded
        conv = conv + filters[k : k + 1, :] * moved[EDGE : EDGE + length]
    act = conv * jax.nn.sigmoid(conv)
    values = act[:, :width]
    bs = [act[:, width + g * states : width + (g + 1) * states].astype(BF16) for g in range(groups)]
    cs = [
        act[:, width + (groups + g) * states : width + (groups + g + 1) * states].astype(BF16)
        for g in range(groups)
    ]
    share = width // groups
    end_row = lax.broadcasted_iota(jnp.int32, (EDGE, width), 0)
    for way, tail, tot in ((0, tail_f, total_f), (1, tail_b, total_b)):
        weighted = (values * tail).astype(BF16)
        for g in range(groups):
            cols = slice(g * share, (g + 1) * share)
            ends[way, 0:states, cols] = narrow_dot(bs[g], weighted[:, cols], ((0,), (0,))).astype(
                BF16
            )
        high = tot.astype(BF16).astype(F32)
        low = tot - high
        ends[way, states : states + EDGE, :] = jnp.where(
            end_row == 0, high, jnp.where(end_row == 1, low, 0.0)
        ).astype(BF16)
    state_copies = []
    for k in range(1, n):
        copy = pltpu.make_async_remote_copy(
            src_ref=ends.at[(d + k) // n],
            dst_ref=got.at[k - 1],
            send_sem=state_send.at[k - 1],
            recv_sem=state_recv.at[k - 1],
            device_id={"sp": lax.rem(d + k, n)},
            device_id_type=MESH,
        )
        copy.start()
        state_copies.append(copy)

    blocks = []
    heads_in = heads // groups
    for g in range(groups):
        scores = narrow_dot(cs[g], bs[g], ((1,), (1,)))
        for h in range(g * heads_in, (g + 1) * heads_in):
            b = heads + h
            spread_f = within[:, h : h + 1] - within_t[h : h + 1, :]
            spread_b = before_t[b : b + 1, :] - before[:, b : b + 1]
            factor = jnp.exp(jnp.where(row_i >= col_i, spread_f, spread_b))
            sf, sb = step_t[h : h + 1, :], step_t[b : b + 1, :]
            coeff = jnp.where(row_i >= col_i, sf, 0.0) + jnp.where(row_i <= col_i, sb, 0.0)
            mat = (scores * factor * coeff).astype(BF16)
            blocks.append(narrow_dot(mat, values[:, h * HD : (h + 1) * HD]))
    out = jnp.concatenate(blocks, axis=1)
    gate = gate_ref[...].astype(F32)
    gate = gate * jax.nn.sigmoid(gate)

    for copy in state_copies:
        copy.wait()
    weight = jnp.where(d >= 1, 1.0, 0.0) * jnp.ones((1, width), F32)
    start_f = jnp.zeros((states, width), F32)
    for k in range(1, n):
        weight = jnp.where(d >= k, weight, 0.0)
        start_f = start_f + weight * got[k - 1, 0:states, :].astype(F32)
        marks = got[k - 1, states : states + EDGE, :].astype(F32)
        weight = weight * jnp.exp(marks[0:1] + marks[1:2])
    weight = jnp.ones((1, width), F32)
    start_b = jnp.zeros((states, width), F32)
    for m in range(1, n):
        weight = jnp.where(d + m < n, weight, 0.0)
        slot = n - m - 1
        start_b = start_b + weight * got[slot, 0:states, :].astype(F32)
        marks = got[slot, states : states + EDGE, :].astype(F32)
        weight = weight * jnp.exp(jnp.minimum(marks[0:1] + marks[1:2], 0.0))
    carried = []
    for g in range(groups):
        cols = slice(g * share, (g + 1) * share)
        carried.append(
            head_f[:, cols] * narrow_dot(cs[g], start_f[:, cols])
            + head_b[:, cols] * narrow_dot(cs[g], start_b[:, cols])
        )
    out = out + (carried[0] if groups == 1 else jnp.concatenate(carried, axis=1))
    gated = out * gate
    square = exact_dot(gated * gated, spread, ((1,), (1,))) * (1.0 / HD)
    scale = widen(lax.rsqrt(square + EPSILON))
    mixed = (gated * scale * gain_ref[...]).astype(BF16)
    model = wout_ref.shape[1]
    tile = min(512, model)
    for c in range(0, model, tile):
        part[:, c : c + tile] = jnp.dot(
            mixed, wout_ref[:, c : c + tile], preferred_element_type=F32
        ).astype(BF16)
    part_copies = []
    for k in range(1, parts):
        target = lax.rem(me + k, parts)
        copy = pltpu.make_async_remote_copy(
            src_ref=part.at[pl.ds(pl.multiple_of(target * rows, rows), rows)],
            dst_ref=part_got.at[k - 1],
            send_sem=part_send.at[k - 1],
            recv_sem=part_recv.at[k - 1],
            device_id={"tp": target},
            device_id_type=MESH,
        )
        copy.start()
        part_copies.append(copy)
    residual = resid_ref[...].astype(F32) + part[
        pl.ds(pl.multiple_of(me * rows, rows), rows), :
    ].astype(F32)
    for k in range(1, parts):
        part_copies[k - 1].wait()
        residual = residual + part_got[k - 1].astype(F32)
    residual = residual.astype(BF16)
    resid_out[...] = residual
    wide = residual.astype(F32)
    mean = jnp.mean(wide * wide, axis=1, keepdims=True)
    normed_out[...] = (wide * lax.rsqrt(mean + EPSILON) * fgain_ref[...]).astype(BF16)
    own_route.wait()
    for copy in route_copies:
        copy.wait()


def remote(src, dst, send, recv, where):
    return pltpu.make_async_remote_copy(
        src_ref=src,
        dst_ref=dst,
        send_sem=send,
        recv_sem=recv,
        device_id=where,
        device_id_type=MESH,
    )


def greet(n, parts, d, me, other):
    barrier = pltpu.get_barrier_semaphore()
    for k in range(1, n // 2):
        pl.semaphore_signal(
            barrier, inc=1, device_id={"sp": lax.rem(d + 2 * k, n)}, device_id_type=MESH
        )
    for k in range(1, parts):
        pl.semaphore_signal(
            barrier, inc=1, device_id={"tp": lax.rem(me + k, parts)}, device_id_type=MESH
        )
    pl.semaphore_signal(barrier, inc=1, device_id={"sp": other}, device_id_type=MESH)
    pl.semaphore_wait(barrier, n // 2 + parts - 1)


def gather_kernel(n, parts, x_ref, out, zs, zr, ts, tr, cs, cr, local_sem):
    d, me = lax.axis_index("sp"), lax.axis_index("tp")
    other = d + 1 - 2 * lax.rem(d, 2)
    chips = n // 2
    greet(n, parts, d, me, other)
    z_copies = [None]
    for k in range(1, chips):
        copy = remote(
            x_ref,
            out.at[d, me],
            zs.at[k - 1],
            zr.at[k - 1],
            {"sp": lax.rem(d + 2 * k, n)},
        )
        copy.start()
        z_copies.append(copy)
    own = pltpu.make_async_copy(x_ref, out.at[d, me], local_sem)
    own.start()
    t_copies = []
    for j in range(chips):
        block = lax.rem(d + n - 2 * j, n)
        if j:
            z_copies[j].wait_recv()
        row = []
        for k in range(1, parts):
            copy = remote(
                out.at[block, me] if j else x_ref,
                out.at[block, me],
                ts.at[j, k - 1],
                tr.at[j, k - 1],
                {"tp": lax.rem(me + k, parts)},
            )
            copy.start()
            row.append(copy)
        t_copies.append(row)
    own.wait()
    c_copies = []
    for j in range(chips):
        block = lax.rem(d + n - 2 * j, n)
        for copy in t_copies[j]:
            copy.wait_recv()
        copy = remote(out.at[block], out.at[block], cs.at[j], cr.at[j], {"sp": other})
        copy.start()
        c_copies.append(copy)
    for copy in z_copies[1:]:
        copy.wait_send()
    for row in t_copies:
        for copy in row:
            copy.wait_send()
    for copy in c_copies:
        copy.wait()


def sum_kernel(
    n,
    parts,
    x_ref,
    resid_ref,
    out_ref,
    c_got,
    paired,
    t_got,
    ready,
    z_got,
    zs,
    zr,
    ts,
    tr,
    cs,
    cr,
):
    d, me = lax.axis_index("sp"), lax.axis_index("tp")
    core = lax.rem(d, 2)
    z = d // 2
    other = d + 1 - 2 * core
    chips = n // 2
    greet(n, parts, d, me, other)
    order = list(range(1, chips)) + [0]
    c_copies = {}
    for k in order:
        chip = lax.rem(z + k, chips)
        copy = remote(
            x_ref.at[2 * chip + 1 - core], c_got.at[k], cs.at[k], cr.at[k], {"sp": other}
        )
        copy.start()
        c_copies[k] = copy
    t_copies = {}
    for k in order:
        chip = lax.rem(z + k, chips)
        c_copies[k].wait_recv()

        def add(t, carry, k=k, chip=chip):
            paired[k, t] = (
                x_ref[2 * chip + core, t].astype(F32) + c_got[k, t].astype(F32)
            ).astype(BF16)
            return carry

        lax.fori_loop(0, parts, add, 0)
        for q in range(1, parts):
            t = lax.rem(me + q, parts)
            copy = remote(
                paired.at[k, t],
                t_got.at[k, q - 1],
                ts.at[k, q - 1],
                tr.at[k, q - 1],
                {"tp": t},
            )
            copy.start()
            t_copies[k, q] = copy
    z_copies = {}
    for k in order:
        total = paired[k, me].astype(F32)
        for q in range(1, parts):
            t_copies[k, q].wait_recv()
            total = total + t_got[k, q - 1].astype(F32)
        if k:
            ready[k - 1] = total.astype(BF16)
            copy = remote(
                ready.at[k - 1],
                z_got.at[k - 1],
                zs.at[k - 1],
                zr.at[k - 1],
                {"sp": lax.rem(d + 2 * k, n)},
            )
            copy.start()
            z_copies[k] = copy
    for k in range(1, chips):
        z_copies[k].wait_recv()
        total = total + z_got[k - 1].astype(F32)
    out_ref[...] = (resid_ref[...].astype(F32) + total).astype(BF16)
    for copy in c_copies.values():
        copy.wait_send()
    for copy in t_copies.values():
        copy.wait_send()
    for copy in z_copies.values():
        copy.wait_send()


def on_device(
    residual_input,
    mixer_value_input,
    gate_preactivation,
    state_projection_input,
    step_preactivation,
    spike_log_decay,
    value_filter_taps,
    state_projection_taps,
    step_size_bias,
    head_log_decay,
    gated_norm_gain,
    mixer_output_weight,
    feedforward_norm_gain,
    routed_expert_index,
    routed_expert_weight,
    routed_gate_weight,
    routed_up_weight,
    routed_down_weight,
    common_gate_weight,
    common_up_weight,
    common_down_weight,
):
    n, parts = (lax.axis_size("sp"), lax.axis_size("tp"))
    seq_rows, width = mixer_value_input.shape
    heads = width // HD
    all_groups, states = state_projection_input.shape[2:]
    per_group = heads * parts // all_groups
    groups = max(1, heads // per_group)
    first_group = lax.axis_index("tp") * heads // per_group
    taps = value_filter_taps.shape[0]
    model = mixer_output_weight.shape[1]
    rows = residual_input.shape[0]
    local_experts = routed_gate_weight.shape[0]
    experts = local_experts * n
    bc = lax.dynamic_slice_in_dim(state_projection_input, first_group, groups, 2)
    bc_taps = lax.dynamic_slice_in_dim(state_projection_taps, first_group, groups, 2)
    joined = jnp.concatenate(
        [mixer_value_input, bc.reshape(seq_rows, 2 * groups * states)], axis=1
    )
    named = routed_expert_index[None] == jnp.arange(experts, dtype=jnp.int32)[:, None, None]
    route = jnp.sum(jnp.where(named, routed_expert_weight[None], 0.0), axis=2)
    cols = joined.shape[1]
    vmem = pl.BlockSpec(memory_space=pltpu.VMEM)
    dma = pltpu.SemaphoreType.DMA
    residual, normed, routes = pl.pallas_call(
        functools.partial(mixer_kernel, n, parts, groups),
        out_shape=(
            jax.ShapeDtypeStruct((rows, model), BF16),
            jax.ShapeDtypeStruct((rows, model), BF16),
            jax.ShapeDtypeStruct((n, experts, seq_rows), F32),
        ),
        in_specs=[vmem] * 13,
        out_specs=(vmem, vmem, vmem),
        scratch_shapes=[
            pltpu.VMEM((2, EDGE, cols), BF16),
            pltpu.VMEM((2, states + EDGE, width), BF16),
            pltpu.VMEM((n - 1, states + EDGE, width), BF16),
            pltpu.VMEM((seq_rows, model), BF16),
            pltpu.VMEM((parts - 1, rows, model), BF16),
            dma((2,)),
            dma((2,)),
            dma((n - 1,)),
            dma((n - 1,)),
            dma((parts - 1,)),
            dma((parts - 1,)),
            dma((n - 1,)),
            dma((n - 1,)),
            dma,
        ],
        compiler_params=pltpu.CompilerParams(collective_id=0, has_side_effects=True),
        name="mixer",
    )(
        joined,
        value_filter_taps,
        bc_taps.reshape(taps, 2 * groups * states),
        step_preactivation.astype(F32).reshape(seq_rows, 2 * heads),
        spike_log_decay.reshape(seq_rows, 2 * heads),
        step_size_bias,
        head_log_decay,
        gate_preactivation,
        gated_norm_gain.reshape(1, width),
        mixer_output_weight,
        residual_input,
        feedforward_norm_gain.reshape(1, model),
        route,
    )
    d = lax.axis_index("sp")
    chips = n // 2
    every = pl.pallas_call(
        functools.partial(gather_kernel, n, parts),
        out_shape=jax.ShapeDtypeStruct((n, parts, rows, model), BF16),
        in_specs=[vmem],
        out_specs=vmem,
        scratch_shapes=[
            dma((chips - 1,)),
            dma((chips - 1,)),
            dma((chips, parts - 1)),
            dma((chips, parts - 1)),
            dma((chips,)),
            dma((chips,)),
            dma,
        ],
        compiler_params=pltpu.CompilerParams(collective_id=1, has_side_effects=True),
        name="gather_rows",
    )(normed).reshape(n * seq_rows, model)
    mine = lax.dynamic_slice_in_dim(every, d * seq_rows, seq_rows, 0)

    def ffn(x, wg, wu, wd, scale):
        gate = jnp.dot(x, wg, preferred_element_type=F32)
        up = jnp.dot(x, wu, preferred_element_type=F32)
        hidden = jax.nn.silu(gate) * up
        if scale is not None:
            hidden = hidden * scale
        return jnp.dot(hidden.astype(BF16), wd, preferred_element_type=F32)

    shared = ffn(mine, common_gate_weight, common_up_weight, common_down_weight, None)
    here = (jnp.arange(n, dtype=jnp.int32) == d)[:, None, None]
    partial = jnp.where(here, shared[None], 0.0)
    for e in range(local_experts):
        scale = lax.dynamic_index_in_dim(routes, d * local_experts + e, 1, keepdims=False)
        partial = partial + ffn(
            every,
            routed_gate_weight[e],
            routed_up_weight[e],
            routed_down_weight[e],
            scale.reshape(n * seq_rows, 1),
        ).reshape(n, seq_rows, model)
    return pl.pallas_call(
        functools.partial(sum_kernel, n, parts),
        out_shape=jax.ShapeDtypeStruct((rows, model), BF16),
        in_specs=[vmem, vmem],
        out_specs=vmem,
        scratch_shapes=[
            pltpu.VMEM((chips, parts, rows, model), BF16),
            pltpu.VMEM((chips, parts, rows, model), BF16),
            pltpu.VMEM((chips, parts - 1, rows, model), BF16),
            pltpu.VMEM((chips - 1, rows, model), BF16),
            pltpu.VMEM((chips - 1, rows, model), BF16),
            dma((chips - 1,)),
            dma((chips - 1,)),
            dma((chips, parts - 1)),
            dma((chips, parts - 1)),
            dma((chips,)),
            dma((chips,)),
        ],
        compiler_params=pltpu.CompilerParams(collective_id=2, has_side_effects=True),
        name="sum_rows",
    )(partial.astype(BF16).reshape(n, parts, rows, model), residual)


def solution(mesh):
    return jax.shard_map(
        on_device,
        mesh=mesh,
        in_specs=(
            P(("sp", "tp"), None),
            P("sp", "tp"),
            P("sp", "tp"),
            P("sp", None, None, None),
            P("sp", None, "tp"),
            P("sp", None, "tp"),
            P(None, "tp"),
            P(),
            P(None, "tp"),
            P(None, "tp"),
            P("tp"),
            P("tp", None),
            P(),
            P("sp", None),
            P("sp", None),
            P("sp", None, "tp"),
            P("sp", None, "tp"),
            P("sp", "tp", None),
            P(None, "tp"),
            P(None, "tp"),
            P("tp", None),
        ),
        out_specs=P(("sp", "tp"), None),
        check_vma=False,
    )
```
